32 devices in a mesh: fs: 8 (over z, core), tp: 4 (over y, x).
Axes of the slice: x: 2, y: 2, z: 4, core: 2. Of those that a mesh axis runs over, the one named last changes fastest.
Arguments:
- rows_later: bfloat16 [6144, 2048], P('fs'), may hold values from -6 to 6
- rows_earlier: bfloat16 [6144, 2048], P('fs'), may hold values from -6 to 6
- out_cotangent: bfloat16 [6144, 4096], P('fs', 'tp'), may hold values from -6 to 6
- gate_proj: bfloat16 [2048, 4096], P('fs', 'tp'), may hold values from -0.125 to 0.125
- up_proj: bfloat16 [2048, 4096], P('fs', 'tp'), may hold values from -0.125 to 0.125
- conv_taps: float32 [3, 4096], P(None, 'tp'), may hold values from -4 to 4
- conv_bias: float32 [4096], P('tp'), may hold values from -3 to 3
- gate_grad_sum: float32 [2048, 4096], P('fs', 'tp'), may hold values from -6 to 6
- up_grad_sum: float32 [2048, 4096], P('fs', 'tp'), may hold values from -6 to 6
- taps_grad_sum: float32 [3, 4096], P(None, 'tp'), may hold values from -6 to 6
- bias_grad_sum: float32 [4096], P('tp'), may hold values from -6 to 6
Outputs:
- hidden_later: bfloat16 [6144, 4096], P('fs', 'tp')
- input_grad: bfloat16 [6144, 2048], P('fs')
- gate_grad_out: float32 [2048, 4096], P('fs', 'tp')
- up_grad_out: float32 [2048, 4096], P('fs', 'tp')
- taps_grad_out: float32 [3, 4096], P(None, 'tp')
- bias_grad_out: float32 [4096], P('tp')
The draws below stay inside these ranges and needn't reach their ends.
All inputs are finite; a program needn't handle non-finite values.
Results may differ from the reference program's by a relative error of at most 0.019.
Values may be sent and summed in bfloat16 or wider, within the bound.
No kernel may reach another device: no remote copies, remote signals or barrier semaphores. Data moves between devices by JAX's collectives and lax.ppermute only.
A program may use at most 128 MiB of HBM per device.

```python
import jax
import jax.numpy as jnp
from jax import lax

D = 2048
FF = 4096
TAPS = 3
TOK_DEV = 768
TOKENS = 6144
N_FS = 8
N_TP = 4


def raised(result, rng, source, target, shards_of, factor):
    owner, partner = [(jnp.arange(result.shape[dim]) // (result.shape[dim] // shards_of)).reshape([-1 if axis == dim else 1 for axis in range(result.ndim)]) for dim in (source, target)]
    chosen = jax.random.permutation(rng, shards_of)[partner]
    strong = (owner == chosen) | (owner == (partner + shards_of // 2) % shards_of)
    return jnp.where(strong, factor * result, result)


def shard_levels(own_key, dims, pieces, low, top_value):
    loudness = 1.0
    for axis_at, shards_of in pieces:
        heights = jax.random.uniform(jax.random.fold_in(jax.random.fold_in(own_key, 6), axis_at), (shards_of,), jnp.float32, low / len(pieces), top_value / len(pieces))
        loudness = loudness * jnp.repeat(jnp.exp(heights), dims[axis_at] // shards_of).reshape((-1,) + (1,) * (len(dims) - 1 - axis_at))
    return loudness


def scatter_about(stream_key, dims, spread, limit, shards=(), kind=jnp.bfloat16):
    values = jax.random.normal(stream_key, dims, jnp.float32) * spread
    if len(shards) > 0:
        values = shard_levels(stream_key, dims, shards, -0.22, 0.18) * values
    return jnp.clip(values, min=-limit, max=limit).astype(kind)


def heavy_noise(own_key, shape, width, reach, pieces, heavy, dtype=jnp.bfloat16):
    result = width * jax.random.normal(own_key, shape, jnp.float32)
    if pieces:
        result = result * shard_levels(own_key, shape, pieces, -0.22, 0.18)
    return jnp.clip(raised(result, jax.random.fold_in(own_key, 3), *heavy), -reach, reach).astype(dtype)


def setup_inputs(seed: int = 0) -> dict:
    key_of = jax.random.split(jax.random.key(seed), 12)
    return {
        "rows_later": scatter_about(key_of[0], (TOKENS, D), 1.0, 6.0, ((0, 8),)),
        "rows_earlier": heavy_noise(key_of[1], (TOKENS, D), 1.0, 6.0, ((0, 8),), (0, 1, 8, 2.0)),
        "out_cotangent": heavy_noise(key_of[2], (TOKENS, FF), 1.0, 6.0, ((0, 8), (1, 4)), (0, 1, 8, 2.0)),
        "gate_proj": scatter_about(key_of[3], (D, FF), D ** -0.5, 0.125, ((0, 8), (1, 4))),
        "up_proj": scatter_about(key_of[4], (D, FF), D ** -0.5, 0.125, ((0, 8), (1, 4))),
        "conv_taps": scatter_about(key_of[5], (TAPS, FF), 0.6, 4.0, ((1, 4),), jnp.float32),
        "conv_bias": scatter_about(key_of[6], (FF,), 0.5, 3.0, ((0, 4),), jnp.float32),
        "gate_grad_sum": scatter_about(key_of[7], (D, FF), 1.0, 6.0, ((0, 8), (1, 4)), jnp.float32),
        "up_grad_sum": scatter_about(key_of[8], (D, FF), 1.0, 6.0, ((0, 8), (1, 4)), jnp.float32),
        "taps_grad_sum": scatter_about(key_of[9], (TAPS, FF), 1.0, 6.0, ((1, 4),), jnp.float32),
        "bias_grad_sum": scatter_about(key_of[10], (FF,), 1.0, 6.0, ((0, 4),), jnp.float32),
    }


def shift_down(values, distance):
    total_len = values.shape[1]
    return jnp.pad(values, ((0, 0), (distance, 0), (0, 0)))[:, :total_len]

def shift_up(values, distance):
    return jnp.pad(values, ((0, 0), (0, distance), (0, 0)))[:, distance:]

def causal_mix(pre_values, conv_taps, conv_bias):
    return conv_taps[0] * shift_down(pre_values, 2) + conv_taps[1] * shift_down(pre_values, 1) + conv_taps[2] * pre_values + conv_bias

def mix_adjoint(mixed_grad, conv_taps):
    return conv_taps[2] * mixed_grad + conv_taps[1] * shift_up(mixed_grad, 1) + conv_taps[0] * shift_up(mixed_grad, 2)

def reference(rows_later, rows_earlier, out_cotangent, gate_proj, up_proj, conv_taps, conv_bias, gate_grad_sum, up_grad_sum, taps_grad_sum, bias_grad_sum):
    stacked_rows = jnp.concatenate([rows_later, rows_earlier], axis=0)
    gate_pre = jnp.dot(stacked_rows, gate_proj, preferred_element_type=jnp.float32).astype(jnp.bfloat16)
    up_value = jnp.dot(stacked_rows, up_proj, preferred_element_type=jnp.float32).astype(jnp.bfloat16)
    gate_pre, up_value = lax.optimization_barrier((gate_pre, up_value))
    gate_float = gate_pre.astype(jnp.float32).reshape(2 * N_FS, TOK_DEV, FF)
    up_float = up_value.astype(jnp.float32).reshape(2 * N_FS, TOK_DEV, FF)
    mixed = causal_mix(gate_float, conv_taps, conv_bias)
    sig_all = jax.nn.sigmoid(mixed)
    activated = mixed * sig_all
    hidden = (activated * up_float).astype(jnp.bfloat16)
    hidden_later = hidden[:N_FS].reshape(TOKENS, FF)
    cotangent = out_cotangent.astype(jnp.float32).reshape(N_FS, TOK_DEV, FF)
    mixed_back = mixed[N_FS:]
    sig_back = sig_all[N_FS:]
    up_grad = (cotangent * activated[N_FS:]).astype(jnp.bfloat16).reshape(TOKENS, FF)
    mixed_grad = cotangent * up_float[N_FS:] * sig_back * (1.0 + mixed_back * (1.0 - sig_back))
    gate_grad = mix_adjoint(mixed_grad, conv_taps).astype(jnp.bfloat16).reshape(TOKENS, FF)
    block_width = FF // N_TP
    total = jnp.zeros((TOKENS, D), jnp.float32)
    for block_index in range(N_TP):
        column_start = block_index * block_width
        column_end = column_start + block_width
        part = jnp.dot(gate_grad[:, column_start:column_end], gate_proj[:, column_start:column_end].T, preferred_element_type=jnp.float32) + jnp.dot(up_grad[:, column_start:column_end], up_proj[:, column_start:column_end].T, preferred_element_type=jnp.float32)
        part = lax.optimization_barrier(part.astype(jnp.bfloat16))
        total = total + part.astype(jnp.float32)
    input_grad = total.astype(jnp.bfloat16)
    grad_scale = lax.rsqrt(jnp.asarray(TOKENS, jnp.float32))
    gate_grad_out = gate_grad_sum + grad_scale * jnp.dot(rows_earlier.T, gate_grad, preferred_element_type=jnp.float32)
    up_grad_out = up_grad_sum + grad_scale * jnp.dot(rows_earlier.T, up_grad, preferred_element_type=jnp.float32)
    gate_back = gate_float[N_FS:]
    tap_terms = jnp.stack([lax.optimization_barrier(jnp.sum(mixed_grad * shift_down(gate_back, 2 - tap_index), axis=(0, 1))) for tap_index in range(TAPS)])
    taps_grad_out = taps_grad_sum + grad_scale * tap_terms
    bias_grad_out = bias_grad_sum + grad_scale * lax.optimization_barrier(jnp.sum(mixed_grad, axis=(0, 1)))
    return (hidden_later, input_grad, gate_grad_out, up_grad_out, taps_grad_out, bias_grad_out)
```

```python
import jax
import jax.numpy as jnp
import numpy as np
from jax import lax
from jax.experimental import pallas as pl
from jax.experimental.pallas import tpu as pltpu
from jax.sharding import PartitionSpec as P

LANES = 128
CHUNKS = 2


def contract_last(left, right):
    return lax.dot_general(
        left, right, (((1,), (1,)), ((), ())), preferred_element_type=jnp.float32
    )


def contract_first(left, right):
    return lax.dot_general(
        left, right, (((0,), (0,)), ((), ())), preferred_element_type=jnp.float32
    )


def exchange(values, axis_name, distance):
    pairs = [(i, i ^ distance) for i in range(lax.axis_size(axis_name))]
    return lax.ppermute(values, axis_name, pairs)


def doubling_sum(values, axis_name):
    distance = 1
    while distance < lax.axis_size(axis_name):
        values = values + exchange(values, axis_name, distance)
        distance *= 2
    return values


def step_bit(axis_name, distance):
    return (lax.axis_index(axis_name) // distance) % 2


def halving_scatter(values, axis_name, distances):
    kept = values
    for distance in distances:
        half = kept.shape[0] // 2
        bit = step_bit(axis_name, distance)
        sent = lax.dynamic_slice_in_dim(kept, (1 - bit) * half, half, 0).astype(jnp.bfloat16)
        own = lax.dynamic_slice_in_dim(kept, bit * half, half, 0).astype(jnp.float32)
        kept = own + exchange(sent, axis_name, distance).astype(jnp.float32)
    return kept.astype(jnp.bfloat16)


def doubling_gather(values, axis_name, distances):
    for distance in reversed(distances):
        other = exchange(values, axis_name, distance)
        low = step_bit(axis_name, distance) == 0
        values = jnp.concatenate(
            [jnp.where(low, values, other), jnp.where(low, other, values)], axis=0
        )
    return values


def pair_kernel(gate_ref, up_ref, paired_ref):
    paired_ref[:, :LANES] = gate_ref[...]
    paired_ref[:, LANES:] = up_ref[...]


def pair_blocks(gate, up, first, blocks):
    rows = gate.shape[0]
    at = lambda j: (0, first + j)
    return pl.pallas_call(
        pair_kernel,
        grid=(blocks,),
        in_specs=[pl.BlockSpec((rows, LANES), at)] * 2,
        out_specs=pl.BlockSpec((rows, 2 * LANES), lambda j: (0, j)),
        out_shape=jax.ShapeDtypeStruct((rows, 2 * LANES * blocks), gate.dtype),
        name="pair_blocks",
    )(gate, up)


def rolled(values, distance):
    total = values.shape[0]
    row = lax.broadcasted_iota(jnp.int32, values.shape, 0)
    moved = pltpu.roll(values, distance % total, 0)
    inside = row >= distance if distance > 0 else row < total + distance
    return jnp.where(inside, moved, 0.0)


def mix_block(pre_ref, taps_ref, bias_ref):
    gate = pre_ref[:, :LANES].astype(jnp.float32)
    up = pre_ref[:, LANES:].astype(jnp.float32)
    down_two, down_one = rolled(gate, 2), rolled(gate, 1)
    taps = [taps_ref[k : k + 1, :] for k in range(3)]
    mixed = taps[0] * down_two + taps[1] * down_one + taps[2] * gate + bias_ref[...]
    return gate, up, down_two, down_one, taps, mixed, jax.nn.sigmoid(mixed)


def backward_kernel(pre_ref, cotangent_ref, taps_ref, bias_ref, grads_ref, terms_ref):
    gate, up, down_two, down_one, taps, mixed, sig = mix_block(pre_ref, taps_ref, bias_ref)
    cotangent = cotangent_ref[...].astype(jnp.float32)
    grads_ref[:, LANES:] = (cotangent * (mixed * sig)).astype(jnp.bfloat16)
    mixed_grad = cotangent * up * sig * (1.0 + mixed * (1.0 - sig))
    gate_grad = (
        taps[2] * mixed_grad + taps[1] * rolled(mixed_grad, -1) + taps[0] * rolled(mixed_grad, -2)
    )
    grads_ref[:, :LANES] = gate_grad.astype(jnp.bfloat16)
    for k, shifted in enumerate((down_two, down_one, gate)):
        terms_ref[k : k + 1, :] = jnp.sum(mixed_grad * shifted, axis=0, keepdims=True)
    terms_ref[3:4, :] = jnp.sum(mixed_grad, axis=0, keepdims=True)


def backward_mix(pre, cotangent, taps, bias, first):
    rows, pair_width = pre.shape
    blocks = pair_width // (2 * LANES)
    at = lambda j: (0, first + j)
    return pl.pallas_call(
        backward_kernel,
        grid=(blocks,),
        in_specs=[
            pl.BlockSpec((rows, 2 * LANES), lambda j: (0, j)),
            pl.BlockSpec((rows, LANES), at),
            pl.BlockSpec((taps.shape[0], LANES), at),
            pl.BlockSpec((1, LANES), at),
        ],
        out_specs=[
            pl.BlockSpec((rows, 2 * LANES), lambda j: (0, j)),
            pl.BlockSpec((4, LANES), lambda j: (0, j)),
        ],
        out_shape=[
            jax.ShapeDtypeStruct(pre.shape, jnp.bfloat16),
            jax.ShapeDtypeStruct((4, pair_width // 2), jnp.float32),
        ],
        name="backward_mix",
    )(pre, cotangent, taps, bias)


def forward_kernel(pre_ref, taps_ref, bias_ref, *refs):
    _, up, _, _, _, mixed, sig = mix_block(pre_ref, taps_ref, bias_ref)
    refs[-1][...] = (mixed * sig * up).astype(jnp.bfloat16)


def forward_mix(pre, taps, bias, first, before):
    rows, pair_width = pre.shape
    at = lambda j: (0, first + j)
    prior = [] if before is None else [before]
    return pl.pallas_call(
        forward_kernel,
        grid=(pair_width // (2 * LANES),),
        in_specs=[
            pl.BlockSpec((rows, 2 * LANES), lambda j: (0, j)),
            pl.BlockSpec((taps.shape[0], LANES), at),
            pl.BlockSpec((1, LANES), at),
        ]
        + [pl.BlockSpec(memory_space=pl.ANY) for _ in prior],
        out_specs=pl.BlockSpec((rows, LANES), at),
        out_shape=jax.ShapeDtypeStruct((rows, taps.shape[1]), jnp.bfloat16),
        input_output_aliases={3: 0} if prior else {},
        name="forward_mix",
    )(pre, taps, bias, *prior)


def add_kernel(scale, summed_ref, gate_ref, up_ref, *refs):
    summed = summed_ref[...].astype(jnp.float32)
    refs[-2][...] = gate_ref[...] + scale * summed[:, :LANES]
    refs[-1][...] = up_ref[...] + scale * summed[:, LANES:]


def add_terms(summed, gate_sum, up_sum, scale, first, before):
    rows, pair_width = summed.shape
    at = lambda j: (0, first + j)
    shape = jax.ShapeDtypeStruct(gate_sum.shape, jnp.float32)
    return pl.pallas_call(
        lambda *refs: add_kernel(scale, *refs),
        grid=(pair_width // (2 * LANES),),
        in_specs=[
            pl.BlockSpec((rows, 2 * LANES), lambda j: (0, j)),
            pl.BlockSpec((rows, LANES), at),
            pl.BlockSpec((rows, LANES), at),
        ]
        + [pl.BlockSpec(memory_space=pl.ANY) for _ in before],
        out_specs=[pl.BlockSpec((rows, LANES), at)] * 2,
        out_shape=[shape, shape],
        input_output_aliases={3: 0, 4: 1} if before else {},
        name="add_terms",
    )(summed, gate_sum, up_sum, *before)


def axis_sum(streams, axis_name, between):
    distances = []
    distance = 1
    while distance < lax.axis_size(axis_name):
        distances.append(distance)
        distance *= 2
    turn = len(distances) // 2
    orders = [distances, distances[turn:] + distances[:turn]]
    summed = [halving_scatter(s, axis_name, o) for s, o in zip(streams, orders)]
    summed, between = lax.optimization_barrier((summed, between))
    return [doubling_gather(s, axis_name, o) for s, o in zip(summed, orders)], between


def on_device(
    rows_later,
    rows_earlier,
    out_cotangent,
    gate_proj,
    up_proj,
    conv_taps,
    conv_bias,
    gate_grad_sum,
    up_grad_sum,
    taps_grad_sum,
    bias_grad_sum,
):
    seq_len = rows_later.shape[0]
    shard_rows, shard_width = gate_proj.shape
    fs_size = lax.axis_size("fs")
    per_chunk = shard_width // LANES // CHUNKS
    scale = np.float32(1.0 / np.sqrt(seq_len * fs_size))
    half = seq_len // 2
    bias_row = conv_bias[None]

    weights = []
    sent = None
    for c in range(CHUNKS):
        paired = pair_blocks(gate_proj, up_proj, c * per_chunk, per_chunk)
        if sent is not None:
            paired, sent = lax.optimization_barrier((paired, sent))
        sent = paired
        weights.append(lax.all_gather(paired, "fs", axis=0, tiled=True))

    def project(rows, weight):
        return jnp.dot(rows, weight, preferred_element_type=jnp.float32).astype(jnp.bfloat16)

    def scatter(term):
        return lax.psum_scatter(term, "fs", scatter_dimension=0, tiled=True)

    def later_mix(c, weight, before):
        pre = project(rows_later, weight)
        return forward_mix(pre, conv_taps, bias_row, c * per_chunk, before)

    partial = None
    hidden_later = None
    terms = []
    summed = []
    for c in range(CHUNKS):
        weight = weights[c]
        if partial is not None:
            weight, partial, hidden_later = lax.optimization_barrier(
                (weight, partial, hidden_later)
            )
        pre = project(rows_earlier, weight)
        grads, taps_part = backward_mix(pre, out_cotangent, conv_taps, bias_row, c * per_chunk)
        terms.append(taps_part)
        if c < CHUNKS - 1:
            summed.append(scatter(contract_first(rows_earlier, grads).astype(jnp.bfloat16)))
            part = contract_last(grads, weight)
            partial = part if partial is None else partial + part
            hidden_later = later_mix(c, weight, hidden_later)
        else:
            streams = []
            for at in (slice(0, half), slice(half, None)):
                stream = contract_last(grads[at], weight)
                stream = stream if partial is None else partial[at] + stream
                streams.append(stream.astype(jnp.bfloat16))
            grads, streams = lax.optimization_barrier((grads, streams))
            summed.append(scatter(contract_first(rows_earlier, grads).astype(jnp.bfloat16)))
    sums = ()
    for c in range(CHUNKS - 1):
        sums = add_terms(summed[c], gate_grad_sum, up_grad_sum, scale, c * per_chunk, sums)
    streams, sums = axis_sum(streams, "tp", sums)
    input_grad = jnp.concatenate(streams, axis=0)
    gate_grad_out, up_grad_out = add_terms(
        summed[-1], gate_grad_sum, up_grad_sum, scale, (CHUNKS - 1) * per_chunk, sums
    )
    hidden_later = later_mix(CHUNKS - 1, weights[-1], hidden_later)
    tap_total = doubling_sum(jnp.concatenate(terms, axis=1), "fs")
    taps_grad_out = taps_grad_sum + scale * tap_total[:-1]
    bias_grad_out = bias_grad_sum + scale * tap_total[-1]
    return (hidden_later, input_grad, gate_grad_out, up_grad_out, taps_grad_out, bias_grad_out)


def solution(mesh):
    placed = (
        P("fs", None),
        P("fs", None),
        P("fs", "tp"),
        P("fs", "tp"),
        P("fs", "tp"),
        P(None, "tp"),
        P("tp"),
        P("fs", "tp"),
        P("fs", "tp"),
        P(None, "tp"),
        P("tp"),
    )
    return jax.shard_map(
        on_device,
        mesh=mesh,
        in_specs=placed,
        out_specs=(
            P("fs", "tp"),
            P("fs", None),
            P("fs", "tp"),
            P("fs", "tp"),
            P(None, "tp"),
            P("tp"),
        ),
        check_vma=False,
    )
```
